32 devices in a mesh: kv: 16 (over z, y, x), tp: 2 (over core).
Axes of the slice: x: 2, y: 2, z: 4, core: 2. Of those that a mesh axis runs over, the one named last changes fastest.
Arguments:
- tokens: bfloat16 [16, 4096], P(None, 'kv'), may hold values from -32 to 32
- attn_gain: float32 [4096], P('kv'), may hold values from 0.1 to 1.9
- w_query: bfloat16 [4096, 4096], P('kv', 'tp'), may hold values from -0.09375 to 0.09375
- w_key: bfloat16 [4096, 4096], P('kv', 'tp'), may hold values from -0.09375 to 0.09375
- w_value: bfloat16 [4096, 4096], P('kv', 'tp'), may hold values from -0.09375 to 0.09375
- key_cache: bfloat16 [16, 2048, 32, 128], P(None, 'kv', 'tp'), may hold values from -128 to 128
- value_cache: bfloat16 [16, 2048, 32, 128], P(None, 'kv', 'tp'), may hold values from -6 to 6
- lengths: int32 [16], replicated, may hold values from 1 to 2048, as said below
- mix_weight: float32 [32], P('tp'), may hold values from 0.3 to 0.8
- head_gain: float32 [128], replicated, may hold values from 0.1 to 1.9
- w_out: bfloat16 [4096, 4096], P('tp', 'kv'), may hold values from -0.09375 to 0.09375
- mixer_gain: float32 [4096], P('kv'), may hold values from 0.1 to 1.9
- w_gate: bfloat16 [4096, 11264], P('kv', 'tp'), may hold values from -0.09375 to 0.09375
- w_up: bfloat16 [4096, 11264], P('kv', 'tp'), may hold values from -0.09375 to 0.09375
- w_down: bfloat16 [11264, 4096], P('tp', 'kv'), may hold values from -0.0546875 to 0.0546875
Outputs:
- layer_out: bfloat16 [16, 4096], P(None, 'kv')
The draws below stay inside these ranges and needn't reach their ends.
Inputs may be any that keep to these rules, and one draw needn't show every extreme that they name: `lengths`: one sequence has exactly 2048 live positions; four or more sequences, a quarter of them or more, have 4 or fewer.
All inputs are finite; a program needn't handle non-finite values.
Results may differ from the reference program's by a relative error of at most 0.017.
Values may be sent and summed in bfloat16 or wider, within the bound.
A program may use at most 64 MiB of HBM per device.

```python
import jax
import jax.numpy as jnp
from jax import lax

D = 4096
H = 32
DH = 64
DV = 128
FF = 11264
BATCH = 16
LENGTH = 2048
N_TP = 2


def draw_tokens(key, part):
    first_key, second_key = jax.random.split(key, 2)
    columns = jnp.arange(D, dtype=jnp.float32) / D
    roughness = jnp.exp(jax.random.uniform(second_key, (D,), jnp.float32, -0.7, 0.7))
    column_scale = 3.0 ** columns * roughness
    base_values = jnp.clip(jax.random.normal(first_key, (BATCH, D), jnp.float32), -4.0, 4.0)
    values = base_values * column_scale[None, :]
    return values.astype(jnp.bfloat16)


def draw_key_cache(key, part):
    first_key = jax.random.fold_in(key, 0)
    values = jnp.clip(jax.random.normal(first_key, (BATCH, LENGTH, H, 2 * DH), jnp.float32) * 1.75, -10.5, 10.5)
    return values.astype(jnp.bfloat16)


def draw_lengths(key, part):
    order_key, short_key, middle_key = jax.random.split(jax.random.fold_in(key, 7), 3)
    short_count = max(4, BATCH // 4)
    rank = jnp.arange(BATCH, dtype=jnp.int32)
    short_values = jax.random.randint(short_key, (BATCH,), 1, 5, dtype=jnp.int32)
    short_values = jnp.where(rank == 1, jnp.int32(1), short_values)
    middle_values = jax.random.randint(middle_key, (BATCH,), LENGTH // 8, LENGTH // 2 + 1, dtype=jnp.int32)
    full_values = jnp.full((BATCH,), LENGTH, dtype=jnp.int32)
    ranked = jnp.where(rank == 0, full_values, jnp.where(rank <= short_count, short_values, middle_values))
    order = jax.random.permutation(order_key, BATCH).astype(jnp.int32)
    return ranked[order].astype(jnp.int32)


def shard_levels(own_key, shape, shards, least, largest):
    gain = 1.0
    for axis_at, shards_of in shards:
        draws = jax.random.uniform(jax.random.fold_in(jax.random.fold_in(own_key, 6), axis_at), (shards_of,), jnp.float32, least / len(shards), largest / len(shards))
        gain = gain * jnp.repeat(jnp.exp(draws), shape[axis_at] // shards_of).reshape((-1,) + (1,) * (len(shape) - 1 - axis_at))
    return gain


def bell_draw(stream_key, shape, scale, reach, pieces=(), kind=jnp.bfloat16):
    entries = scale * jax.random.normal(stream_key, shape, jnp.float32)
    if pieces:
        entries = entries * shard_levels(stream_key, shape, pieces, -0.22, 0.18)
    return jnp.clip(entries, -reach, reach).astype(kind)


def setup_inputs(seed: int = 0) -> dict:
    arg_keys = jax.random.split(jax.random.key(seed), 16)
    tokens = draw_tokens(jax.random.fold_in(arg_keys[15], 71), 0)
    attn_gain = jnp.clip(1.0 + 0.18 * jax.random.normal(arg_keys[1], (D,), jnp.float32), 0.1, 1.9)
    w_query = bell_draw(arg_keys[2], (D, H * 2 * DH), D ** -0.5, 0.09375, ((0, 16), (1, 2)))
    w_key = bell_draw(arg_keys[3], (D, H * 2 * DH), D ** -0.5, 0.09375, ((0, 16), (1, 2)))
    w_value = bell_draw(arg_keys[4], (D, H * DV), D ** -0.5, 0.09375, ((0, 16), (1, 2)))
    key_cache = draw_key_cache(jax.random.fold_in(arg_keys[15], 71), 0)
    value_cache = bell_draw(arg_keys[6], (BATCH, LENGTH, H, DV), 1.0, 6.0, ((1, 16), (2, 2)))
    lengths = draw_lengths(jax.random.fold_in(arg_keys[15], 71), 0)
    mix_weight = jnp.clip(0.3 + 0.5 * jax.random.uniform(arg_keys[8], (H,), jnp.float32) ** shard_levels(arg_keys[8], (H,), ((0, 2),), -0.2, 0.2), 0.3, 0.8)
    head_gain = jnp.clip(1.0 + 0.18 * jax.random.normal(arg_keys[9], (DV,), jnp.float32), 0.1, 1.9)
    w_out = bell_draw(arg_keys[10], (H * DV, D), (H * DV) ** -0.5, 0.09375, ((0, 2), (1, 16)))
    mixer_gain = jnp.clip(1.0 + 0.18 * jax.random.normal(arg_keys[11], (D,), jnp.float32), 0.1, 1.9)
    w_gate = bell_draw(arg_keys[12], (D, FF), D ** -0.5, 0.09375, ((0, 16), (1, 2)))
    w_up = bell_draw(arg_keys[13], (D, FF), D ** -0.5, 0.09375, ((0, 16), (1, 2)))
    w_down = bell_draw(arg_keys[14], (FF, D), FF ** -0.5, 0.0546875, ((0, 2), (1, 16)))
    return dict(tokens=tokens, attn_gain=attn_gain, w_query=w_query, w_key=w_key, w_value=w_value, key_cache=key_cache, value_cache=value_cache, lengths=lengths, mix_weight=mix_weight, head_gain=head_gain, w_out=w_out, mixer_gain=mixer_gain, w_gate=w_gate, w_up=w_up, w_down=w_down)


EPS = 1e-06

def rounded(values):
    return lax.optimization_barrier(values.astype(jnp.bfloat16)).astype(jnp.float32)

def one_sequence(queries, key_new, value_new, key_rows, value_rows, seq_length, mix_weight, head_gain):
    logit_scale = DH ** (-0.5)
    query_float = queries.astype(jnp.float32).reshape(H, 2, DH)
    keys_float = key_rows.astype(jnp.float32).reshape(LENGTH, H, 2, DH)
    score_matrix = jnp.einsum('crx,ecrx->cre', query_float, keys_float) * logit_scale
    own_score = lax.optimization_barrier(jnp.sum(query_float * key_new.astype(jnp.float32).reshape(H, 2, DH), axis=2)) * logit_scale
    visible = (jnp.arange(LENGTH, dtype=jnp.int32) < seq_length)[None, None, :]
    peak_score = jnp.maximum(lax.optimization_barrier(jnp.max(jnp.where(visible, score_matrix, -jnp.inf), axis=2)), own_score)
    weights = jnp.where(visible, jnp.exp(score_matrix - peak_score[:, :, None]), 0.0)
    own_weight = jnp.exp(own_score - peak_score)
    totals = lax.optimization_barrier(jnp.sum(weights, axis=2)) + own_weight
    accumulated = jnp.einsum('hmp,phv->hmv', rounded(weights), value_rows.astype(jnp.float32))
    accumulated = accumulated + rounded(own_weight)[:, :, None] * value_new.astype(jnp.float32).reshape(H, 1, DV)
    mixture = accumulated[:, 0] / totals[:, 0, None] - mix_weight[:, None] * accumulated[:, 1] / totals[:, 1, None]
    head_scale = lax.rsqrt(lax.optimization_barrier(jnp.mean(mixture * mixture, axis=1, keepdims=True)) + EPS)
    return (mixture * head_scale * head_gain.astype(jnp.float32)).astype(jnp.bfloat16).reshape(H * DV)

def blocked_sum(left_side, right_side, group_count):
    row_count = left_side.shape[0]
    inner_size = left_side.shape[1] // group_count
    partial_terms = jnp.einsum('bgi,gid->gbd', left_side.astype(jnp.float32).reshape(row_count, group_count, inner_size), right_side.astype(jnp.float32).reshape(group_count, inner_size, right_side.shape[1]))
    return lax.optimization_barrier(jnp.sum(rounded(partial_terms), axis=0))

def reference(tokens, attn_gain, w_query, w_key, w_value, key_cache, value_cache, lengths, mix_weight, head_gain, w_out, mixer_gain, w_gate, w_up, w_down):
    tokens_float = tokens.astype(jnp.float32)
    inverse = lax.rsqrt(lax.optimization_barrier(jnp.mean(tokens_float * tokens_float, axis=1, keepdims=True)) + EPS)
    scaled = (tokens_float * attn_gain.astype(jnp.float32)).astype(jnp.bfloat16)
    queries = (inverse * jnp.dot(scaled, w_query, preferred_element_type=jnp.float32)).astype(jnp.bfloat16)
    key_new = (inverse * jnp.dot(scaled, w_key, preferred_element_type=jnp.float32)).astype(jnp.bfloat16)
    value_new = (inverse * jnp.dot(scaled, w_value, preferred_element_type=jnp.float32)).astype(jnp.bfloat16)

    def per_sequence(inputs):
        return one_sequence(inputs[0], inputs[1], inputs[2], inputs[3], inputs[4], inputs[5], mix_weight.astype(jnp.float32), head_gain)
    attended = lax.map(per_sequence, (queries, key_new, value_new, key_cache, value_cache, lengths.astype(jnp.int32)))
    residual = (tokens_float + blocked_sum(attended, w_out, N_TP)).astype(jnp.bfloat16)
    residual_f = residual.astype(jnp.float32)
    reciprocal_mixture = lax.rsqrt(lax.optimization_barrier(jnp.mean(residual_f * residual_f, axis=1, keepdims=True)) + EPS)
    scaled_mix = (residual_f * mixer_gain.astype(jnp.float32)).astype(jnp.bfloat16)
    gate = reciprocal_mixture * jnp.dot(scaled_mix, w_gate, preferred_element_type=jnp.float32)
    up_proj = reciprocal_mixture * jnp.dot(scaled_mix, w_up, preferred_element_type=jnp.float32)
    hidden = (jax.nn.silu(gate) * up_proj).astype(jnp.bfloat16)
    return (residual_f + blocked_sum(hidden, w_down, N_TP)).astype(jnp.bfloat16)
```

```python
import functools

import jax
import jax.numpy as jnp
from jax import lax
from jax.experimental import pallas as pl
from jax.experimental.pallas import tpu as pltpu
from jax.sharding import PartitionSpec as P

EPS = 1e-06
FLOOR_SCORE = -1e30
LANES = 128
F32 = jnp.float32
BF16 = jnp.bfloat16
VMEM = pl.BlockSpec(memory_space=pltpu.VMEM)
SMEM = pl.BlockSpec(memory_space=pltpu.SMEM)
ANY = pl.BlockSpec(memory_space=pl.ANY)


def greet(n, me, others=()):
    barrier = pltpu.get_barrier_semaphore()
    for i in range(1, n):
        pl.semaphore_signal(
            barrier,
            inc=1,
            device_id={"kv": lax.rem(me + i, n)},
            device_id_type=pl.DeviceIdType.MESH,
        )
    for other in others:
        pl.semaphore_signal(
            barrier, inc=1, device_id={"tp": other}, device_id_type=pl.DeviceIdType.MESH
        )
    return barrier, n - 1 + len(others)


def landed(buf, recv, k):
    pltpu.make_async_copy(buf.at[k], buf.at[k], recv.at[k]).wait()


def remote(src, dst, send_sem, recv_sem, target):
    return pltpu.make_async_remote_copy(
        src_ref=src,
        dst_ref=dst,
        send_sem=send_sem,
        recv_sem=recv_sem,
        device_id=target,
        device_id_type=pl.DeviceIdType.MESH,
    )


def each_owner(n, owners, me, body):
    for i in range(owners):
        if owners == n:
            if i > 0:
                body(lax.rem(me + i, n))
        else:
            o = lax.rem(me + i, owners)
            pl.when(o != me)(functools.partial(body, o))


def when_owner(n, owners, me, body):
    if owners == n:
        body()
    else:
        pl.when(me < owners)(body)


def project_kernel(
    n, heads, width, tokens, gain, wq, wk, wv, q_out, own_out,
    sbuf, rbuf, gsrc, gbuf, send, recv,
):
    me = lax.axis_index("kv")
    barrier, count = greet(n, me)
    tokens_f = tokens[...].astype(F32)
    scaled = (tokens_f * gain[...]).astype(BF16)
    squares = jnp.sum(tokens_f * tokens_f, axis=1, keepdims=True)
    squares = jnp.broadcast_to(squares, (tokens.shape[0], LANES))
    for j, w in enumerate((wq, wk, wv)):
        part = jnp.dot(scaled, w[...], preferred_element_type=F32)
        for h in range(heads):
            sbuf[h, j] = part[:, h * LANES : (h + 1) * LANES]
    for h in range(heads):
        sbuf[h, 3] = squares
    pl.semaphore_wait(barrier, count)

    def reduce_copy(o):
        return remote(sbuf.at[o], rbuf.at[me], send.at[0, o], recv.at[0, me], {"kv": o})

    def gather_copy(o):
        return remote(gsrc, gbuf.at[me], send.at[1, o], recv.at[1, me], {"kv": o})

    each_owner(n, heads, me, lambda o: reduce_copy(o).start())

    def own():
        rbuf[me] = sbuf[me]
        for i in range(1, n):
            landed(rbuf, recv.at[0], lax.rem(me + n - i, n))
        total = rbuf[0]
        for k in range(1, n):
            total = total + rbuf[k]
        inverse = lax.rsqrt(total[3] / width + EPS)
        for j in range(3):
            own_out[j] = (inverse * total[j]).astype(BF16)
        gsrc[...] = (inverse * total[0]).astype(BF16)
        for i in range(1, n):
            gather_copy(lax.rem(me + i, n)).start()
        gbuf[me] = (inverse * total[0]).astype(BF16)

    when_owner(n, heads, me, own)
    each_owner(n, heads, me, lambda o: landed(gbuf, recv.at[1], o))
    q_out[...] = gbuf[...]
    each_owner(n, heads, me, lambda o: reduce_copy(o).wait_send())

    def drain():
        for i in range(1, n):
            gather_copy(lax.rem(me + i, n)).wait_send()

    when_owner(n, heads, me, drain)


def attend_kernel(heads, scale, info, q_ref, k_ref, v_ref, value_out, lse_out):
    b = pl.program_id(0)
    live = info[1, b]
    rows = 2 * heads

    @pl.when(live > 0)
    def _():
        q = q_ref[0]
        lane = lax.broadcasted_iota(jnp.int32, q.shape, 1)
        half = q.shape[1] // 2
        zero = jnp.zeros_like(q)
        queries = jnp.concatenate(
            [jnp.where(lane < half, q, zero), jnp.where(lane >= half, q, zero)], axis=0
        )
        keys = k_ref[0].reshape(-1, k_ref.shape[3])
        values = v_ref[0].reshape(-1, v_ref.shape[3])
        scores = lax.dot_general(
            queries, keys, (((1,), (1,)), ((), ())), preferred_element_type=F32
        )
        column = lax.broadcasted_iota(jnp.int32, scores.shape, 1)
        row = lax.broadcasted_iota(jnp.int32, scores.shape, 0)
        visible = (lax.rem(column, heads) == lax.rem(row, heads)) & (column < live * heads)
        scores = jnp.where(visible, scores * scale, FLOOR_SCORE)
        peak = jnp.max(scores, axis=1, keepdims=True)
        weights = jnp.where(visible, jnp.exp(scores - peak), 0.0)
        totals = jnp.sum(weights, axis=1, keepdims=True)
        position = lax.broadcasted_iota(jnp.int32, values.shape, 0)
        values = jnp.where(position < live * heads, values, jnp.zeros_like(values))
        summed = jnp.dot(weights.astype(BF16), values, preferred_element_type=F32)
        value_out[0] = (summed / totals).astype(BF16)
        lse_out[0] = jnp.broadcast_to(peak + jnp.log(totals), (rows, LANES))

    @pl.when(live <= 0)
    def _():
        value_out[0] = jnp.zeros(value_out.shape[1:], BF16)
        lse_out[0] = jnp.full((rows, LANES), FLOOR_SCORE, F32)


def finish_kernel(
    n, team, heads, owners, tile, width, scale,
    vals, lses, own_qkv, mix, head_gain, tokens, mixer_gain, w_out, w_gate, w_up, w_down,
    out,
    wo, wg, wu, wd, rvals, rlses, asrc, agat, xsrc, xdst, ssrc, sdst,
    gsrc, gdst, hsrc, hgat, ysrc, ydst, send, recv, tsend, trecv, load,
):
    me = lax.axis_index("kv")
    mate = lax.axis_index("tp")
    mates = [lax.rem(mate + i, team) for i in range(1, team)]
    barrier, count = greet(n, me, mates)
    hidden_width = w_gate.shape[1]
    loads = [
        pltpu.make_async_copy(w_out, wo, load.at[0]),
        pltpu.make_async_copy(w_gate, wg.at[:, pl.ds(0, hidden_width)], load.at[1]),
        pltpu.make_async_copy(w_up, wu.at[:, pl.ds(0, hidden_width)], load.at[2]),
        pltpu.make_async_copy(w_down, wd, load.at[3]),
    ]
    for copy in loads:
        copy.start()
    padded = owners * tile
    if padded > hidden_width:
        for w in (wg, wu):
            w[:, pl.ds(hidden_width, padded - hidden_width)] = jnp.zeros(
                (w.shape[0], padded - hidden_width), BF16
            )
    pl.semaphore_wait(barrier, count)

    def vals_copy(o):
        return remote(vals.at[o], rvals.at[me], send.at[0, o], recv.at[0, me], {"kv": o})

    def lses_copy(o):
        return remote(lses.at[o], rlses.at[me], send.at[1, o], recv.at[1, me], {"kv": o})

    def attended_copy(o):
        return remote(asrc, agat.at[me], send.at[2, o], recv.at[2, me], {"kv": o})

    def start_parts(o):
        lses_copy(o).start()
        vals_copy(o).start()

    each_owner(n, heads, me, start_parts)

    def own_head():
        rvals[me] = vals[me]
        rlses[me] = lses[me]
        q, k, v = (own_qkv[j].astype(F32) for j in range(3))
        product = q * k
        lane = lax.broadcasted_iota(jnp.int32, product.shape, 1)
        half = product.shape[1] // 2
        own_scores = [
            jnp.sum(jnp.where(side, product, 0.0), axis=1, keepdims=True) * scale
            for side in (lane < half, lane >= half)
        ]
        for i in range(1, n):
            landed(rlses, recv.at[1], lax.rem(me + n - i, n))
            landed(rvals, recv.at[0], lax.rem(me + n - i, n))
        normed = []
        for m in range(2):
            own_score = jnp.broadcast_to(own_scores[m], v.shape)
            peak = own_score
            for j in range(n):
                peak = jnp.maximum(peak, rlses[j, m])
            own_weight = jnp.exp(own_score - peak)
            totals = own_weight
            summed = own_weight.astype(BF16).astype(F32) * v
            for j in range(n):
                weight = jnp.exp(rlses[j, m] - peak)
                totals = totals + weight
                summed = summed + weight * rvals[j, m].astype(F32)
            normed.append(summed / totals)
        mixture = normed[0] - mix[0, me] * normed[1]
        head_scale = lax.rsqrt(jnp.mean(mixture * mixture, axis=1, keepdims=True) + EPS)
        attended = (mixture * head_scale * head_gain[...]).astype(BF16)
        asrc[...] = attended
        for i in range(1, n):
            attended_copy(lax.rem(me + i, n)).start()
        agat[me] = attended

    when_owner(n, heads, me, own_head)
    loads[0].wait()
    each_owner(n, heads, me, lambda o: landed(agat, recv.at[2], o))
    attended_all = jnp.concatenate([agat[h] for h in range(heads)], axis=1)
    part = jnp.dot(attended_all, wo[...], preferred_element_type=F32).astype(BF16)
    xsrc[...] = part

    def swap_copy(src, dst, phase, other):
        return remote(
            src, dst.at[mate], tsend.at[phase, other], trecv.at[phase, mate], {"tp": other}
        )

    def team_sum(src, dst, phase):
        for other in mates:
            swap_copy(src, dst, phase, other).start()
        total = src[...].astype(F32)
        for other in mates:
            landed(dst, trecv.at[phase], other)
            total = total + dst[other].astype(F32)
        return total

    residual = (tokens[...].astype(F32) + team_sum(xsrc, xdst, 0)).astype(BF16)
    residual_f = residual.astype(F32)
    scaled_mix = (residual_f * mixer_gain[...]).astype(BF16)
    squares = jnp.sum(residual_f * residual_f, axis=1, keepdims=True)
    ssrc[...] = jnp.broadcast_to(squares, ssrc.shape)

    def squares_copy(o):
        return remote(ssrc, sdst.at[me], send.at[3, o], recv.at[3, me], {"kv": o})

    def gate_copy(o):
        return remote(gsrc.at[o], gdst.at[me], send.at[4, o], recv.at[4, me], {"kv": o})

    def hidden_copy(o):
        return remote(hsrc, hgat.at[me], send.at[5, o], recv.at[5, me], {"kv": o})

    loads[1].wait()
    loads[2].wait()
    each_owner(n, owners, me, lambda o: squares_copy(o).start())
    for i in range(owners):
        o = lax.rem(me + 1 + i, owners)
        columns = pl.ds(pl.multiple_of(o * tile, LANES), tile)
        for j, w in enumerate((wg, wu)):
            gsrc[o, j] = jnp.dot(
                scaled_mix, w[:, columns], preferred_element_type=F32
            ).astype(BF16)
        pl.when(o != me)(lambda: gate_copy(o).start())

    def own_hidden():
        sdst[me] = ssrc[...]
        gdst[me] = gsrc[me]
        for i in range(1, n):
            landed(sdst, recv.at[3], lax.rem(me + n - i, n))
            landed(gdst, recv.at[4], lax.rem(me + n - i, n))
        total = sdst[0]
        for j in range(1, n):
            total = total + sdst[j]
        inverse = lax.rsqrt(total[:, :1] / width + EPS)
        gate = gdst[0, 0].astype(F32)
        up = gdst[0, 1].astype(F32)
        for j in range(1, n):
            gate = gate + gdst[j, 0].astype(F32)
            up = up + gdst[j, 1].astype(F32)
        gate = inverse * gate
        hidden = (gate / (1.0 + jnp.exp(-gate)) * (inverse * up)).astype(BF16)
        hsrc[...] = hidden
        for i in range(1, n):
            hidden_copy(lax.rem(me + i, n)).start()
        hgat[me] = hidden

    when_owner(n, owners, me, own_hidden)
    loads[3].wait()
    each_owner(n, owners, me, lambda o: landed(hgat, recv.at[5], o))
    hidden_all = jnp.concatenate([hgat[o] for o in range(owners)], axis=1)[:, :hidden_width]
    down = jnp.dot(hidden_all, wd[...], preferred_element_type=F32).astype(BF16)
    ysrc[...] = down
    out[...] = (residual_f + team_sum(ysrc, ydst, 1)).astype(BF16)

    each_owner(n, heads, me, lambda o: vals_copy(o).wait_send())
    each_owner(n, heads, me, lambda o: lses_copy(o).wait_send())
    for other in mates:
        swap_copy(xsrc, xdst, 0, other).wait_send()
        swap_copy(ysrc, ydst, 1, other).wait_send()
    each_owner(n, owners, me, lambda o: squares_copy(o).wait_send())
    each_owner(n, owners, me, lambda o: gate_copy(o).wait_send())

    def drain(copy):
        for i in range(1, n):
            copy(lax.rem(me + i, n)).wait_send()

    when_owner(n, heads, me, lambda: drain(attended_copy))
    when_owner(n, owners, me, lambda: drain(hidden_copy))


def local(
    n, team, tokens, attn_gain, w_query, w_key, w_value, key_cache, value_cache, lengths,
    mix_weight, head_gain, w_out, mixer_gain, w_gate, w_up, w_down,
):
    seqs, span_width = tokens.shape
    heads = mix_weight.shape[0]
    span = key_cache.shape[1]
    scale = (key_cache.shape[3] // 2) ** -0.5
    width = span_width * n
    hidden_width = w_gate.shape[1]
    tiles = hidden_width // LANES
    tile = -(-tiles // n)
    owners = -(-tiles // tile)
    tile *= LANES
    remote_params = functools.partial(
        pltpu.CompilerParams, has_side_effects=True, vmem_limit_bytes=60 * 2**20
    )

    queries, own_qkv = pl.pallas_call(
        functools.partial(project_kernel, n, heads, width),
        out_shape=(
            jax.ShapeDtypeStruct((heads, seqs, LANES), BF16),
            jax.ShapeDtypeStruct((3, seqs, LANES), BF16),
        ),
        in_specs=[VMEM] * 5,
        out_specs=(VMEM, VMEM),
        scratch_shapes=[
            pltpu.VMEM((heads, 4, seqs, LANES), F32),
            pltpu.VMEM((n, 4, seqs, LANES), F32),
            pltpu.VMEM((seqs, LANES), BF16),
            pltpu.VMEM((heads, seqs, LANES), BF16),
            pltpu.SemaphoreType.DMA((2, n)),
            pltpu.SemaphoreType.DMA((2, n)),
        ],
        compiler_params=remote_params(collective_id=0),
        name="project",
    )(tokens, attn_gain[None], w_query, w_key, w_value)

    live = lengths - lax.axis_index("kv") * span
    order = jnp.arange(seqs, dtype=jnp.int32)
    seen = (order[None, :] <= order[:, None]) & (live > 0)[None, :]
    fetch = jnp.max(jnp.where(seen, order[None, :], 0), axis=1)
    info = jnp.stack([fetch, live])

    cache_spec = pl.BlockSpec(
        (1, *key_cache.shape[1:]), lambda b, info: (info[0, b], 0, 0, 0)
    )
    part_spec = pl.BlockSpec((1, 2 * heads, LANES), lambda b, info: (b, 0, 0))
    values, lses = pl.pallas_call(
        functools.partial(attend_kernel, heads, scale),
        out_shape=(
            jax.ShapeDtypeStruct((seqs, 2 * heads, LANES), BF16),
            jax.ShapeDtypeStruct((seqs, 2 * heads, LANES), F32),
        ),
        grid_spec=pltpu.PrefetchScalarGridSpec(
            num_scalar_prefetch=1,
            grid=(seqs,),
            in_specs=[
                pl.BlockSpec((1, heads, LANES), lambda b, info: (b, 0, 0)),
                cache_spec,
                cache_spec,
            ],
            out_specs=(part_spec, part_spec),
        ),
        compiler_params=pltpu.CompilerParams(
            dimension_semantics=("arbitrary",), vmem_limit_bytes=60 * 2**20
        ),
        name="attend",
    )(info, queries.transpose(1, 0, 2), key_cache, value_cache)

    def by_head(array):
        return array.reshape(seqs, 2, heads, LANES).transpose(2, 1, 0, 3)

    return pl.pallas_call(
        functools.partial(finish_kernel, n, team, heads, owners, tile, width, scale),
        out_shape=jax.ShapeDtypeStruct((seqs, span_width), BF16),
        in_specs=[VMEM, VMEM, VMEM, SMEM, VMEM, VMEM, VMEM, ANY, ANY, ANY, ANY],
        out_specs=VMEM,
        scratch_shapes=[
            pltpu.VMEM(w_out.shape, BF16),
            pltpu.VMEM((span_width, owners * tile), BF16),
            pltpu.VMEM((span_width, owners * tile), BF16),
            pltpu.VMEM(w_down.shape, BF16),
            pltpu.VMEM((n, 2, seqs, LANES), BF16),
            pltpu.VMEM((n, 2, seqs, LANES), F32),
            pltpu.VMEM((seqs, LANES), BF16),
            pltpu.VMEM((heads, seqs, LANES), BF16),
            pltpu.VMEM((seqs, span_width), BF16),
            pltpu.VMEM((team, seqs, span_width), BF16),
            pltpu.VMEM((seqs, LANES), F32),
            pltpu.VMEM((n, seqs, LANES), F32),
            pltpu.VMEM((owners, 2, seqs, tile), BF16),
            pltpu.VMEM((n, 2, seqs, tile), BF16),
            pltpu.VMEM((seqs, tile), BF16),
            pltpu.VMEM((owners, seqs, tile), BF16),
            pltpu.VMEM((seqs, span_width), BF16),
            pltpu.VMEM((team, seqs, span_width), BF16),
            pltpu.SemaphoreType.DMA((6, n)),
            pltpu.SemaphoreType.DMA((6, n)),
            pltpu.SemaphoreType.DMA((2, team)),
            pltpu.SemaphoreType.DMA((2, team)),
            pltpu.SemaphoreType.DMA((4,)),
        ],
        compiler_params=remote_params(collective_id=1),
        name="finish",
    )(
        by_head(values), by_head(lses), own_qkv, mix_weight[None], head_gain[None],
        tokens, mixer_gain[None], w_out, w_gate, w_up, w_down,
    )


def solution(mesh):
    return jax.shard_map(
        functools.partial(local, mesh.shape["kv"], mesh.shape["tp"]),
        mesh=mesh,
        in_specs=(
            P(None, "kv"),
            P("kv"),
            P("kv", "tp"),
            P("kv", "tp"),
            P("kv", "tp"),
            P(None, "kv", "tp", None),
            P(None, "kv", "tp", None),
            P(),
            P("tp"),
            P(),
            P("tp", "kv"),
            P("kv"),
            P("kv", "tp"),
            P("kv", "tp"),
            P("tp", "kv"),
        ),
        out_specs=P(None, "kv"),
        check_vma=False,
    )
```

```python
import functools

import jax
import jax.numpy as jnp
from jax import lax
from jax.experimental import pallas as pl
from jax.experimental.pallas import tpu as pltpu
from jax.sharding import PartitionSpec as P

EPS = 1e-06
FLOOR_SCORE = -1e30
LANES = 128
F32 = jnp.float32
BF16 = jnp.bfloat16
VMEM = pl.BlockSpec(memory_space=pltpu.VMEM)
SMEM = pl.BlockSpec(memory_space=pltpu.SMEM)
ANY = pl.BlockSpec(memory_space=pl.ANY)


def greet(n, me, others=()):
    barrier = pltpu.get_barrier_semaphore()
    for i in range(1, n):
        pl.semaphore_signal(
            barrier,
            inc=1,
            device_id={"kv": lax.rem(me + i, n)},
            device_id_type=pl.DeviceIdType.MESH,
        )
    for other in others:
        pl.semaphore_signal(
            barrier, inc=1, device_id={"tp": other}, device_id_type=pl.DeviceIdType.MESH
        )
    return barrier, n - 1 + len(others)


def landed(buf, recv, k):
    pltpu.make_async_copy(buf.at[k], buf.at[k], recv.at[k]).wait()


def remote(src, dst, send_sem, recv_sem, target):
    return pltpu.make_async_remote_copy(
        src_ref=src,
        dst_ref=dst,
        send_sem=send_sem,
        recv_sem=recv_sem,
        device_id=target,
        device_id_type=pl.DeviceIdType.MESH,
    )


def diagonal(seqs):
    lane = lax.broadcasted_iota(jnp.int32, (seqs, LANES), 1)
    return lane == lax.broadcasted_iota(jnp.int32, (seqs, LANES), 0)


def to_lanes(column):
    seqs = column.shape[0]
    spread = jnp.where(diagonal(seqs), jnp.broadcast_to(column, (seqs, LANES)), 0.0)
    return jnp.broadcast_to(jnp.sum(spread, axis=0, keepdims=True), (8, LANES))


def to_rows(row, seqs):
    spread = jnp.where(diagonal(seqs), jnp.broadcast_to(row, (seqs, LANES)), 0.0)
    return jnp.sum(spread, axis=1, keepdims=True)


def each_owner(n, owners, me, body):
    for i in range(owners):
        if owners == n:
            if i > 0:
                body(lax.rem(me + i, n))
        else:
            o = lax.rem(me + i, owners)
            pl.when(o != me)(functools.partial(body, o))


def when_owner(n, owners, me, body):
    if owners == n:
        body()
    else:
        pl.when(me < owners)(body)


def project_kernel(
    n, heads, width, tokens, gain, wq, wk, wv, q_out, own_out,
    wbuf, sbuf, rbuf, nsrc, ndst, gsrc, gbuf, send, recv, load,
):
    me = lax.axis_index("kv")
    barrier, count = greet(n, me)
    loads = [
        pltpu.make_async_copy(w, wbuf.at[j], load.at[j]) for j, w in enumerate((wq, wk, wv))
    ]
    for copy in loads:
        copy.start()
    tokens_f = tokens[...].astype(F32)
    scaled = (tokens_f * gain[...]).astype(BF16)
    squares = jnp.sum(tokens_f * tokens_f, axis=1, keepdims=True)
    nsrc[...] = to_lanes(squares)
    for j, copy in enumerate(loads):
        copy.wait()
        part = jnp.dot(scaled, wbuf[j], preferred_element_type=F32).astype(BF16)
        for h in range(heads):
            sbuf[h, j] = part[:, h * LANES : (h + 1) * LANES]
    pl.semaphore_wait(barrier, count)

    def reduce_copy(o):
        return remote(sbuf.at[o], rbuf.at[me], send.at[0, o], recv.at[0, me], {"kv": o})

    def gather_copy(o):
        return remote(gsrc, gbuf.at[me], send.at[1, o], recv.at[1, me], {"kv": o})

    def norm_copy(o):
        return remote(nsrc, ndst.at[me], send.at[2, o], recv.at[2, me], {"kv": o})

    def start_parts(o):
        norm_copy(o).start()
        reduce_copy(o).start()

    each_owner(n, heads, me, start_parts)

    def own():
        rbuf[me] = sbuf[me]
        ndst[me] = nsrc[...]
        for i in range(1, n):
            landed(ndst, recv.at[2], lax.rem(me + n - i, n))
            landed(rbuf, recv.at[0], lax.rem(me + n - i, n))
        total = rbuf[0].astype(F32)
        norm = ndst[0]
        for k in range(1, n):
            total = total + rbuf[k].astype(F32)
            norm = norm + ndst[k]
        inverse = lax.rsqrt(to_rows(norm[:1], tokens.shape[0]) / width + EPS)
        for j in range(3):
            own_out[j] = (inverse * total[j]).astype(BF16)
        gsrc[...] = (inverse * total[0]).astype(BF16)
        for i in range(1, n):
            gather_copy(lax.rem(me + i, n)).start()
        gbuf[me] = (inverse * total[0]).astype(BF16)

    when_owner(n, heads, me, own)
    each_owner(n, heads, me, lambda o: landed(gbuf, recv.at[1], o))
    q_out[...] = gbuf[...]
    each_owner(n, heads, me, lambda o: reduce_copy(o).wait_send())
    each_owner(n, heads, me, lambda o: norm_copy(o).wait_send())

    def drain():
        for i in range(1, n):
            gather_copy(lax.rem(me + i, n)).wait_send()

    when_owner(n, heads, me, drain)


def attend_kernel(heads, scale, info, q_ref, k_ref, v_ref, value_out, lse_out):
    b = pl.program_id(0)
    live = info[1, b]
    slot = lax.broadcasted_iota(jnp.int32, lse_out.shape, 1) == b

    @pl.when(b == 0)
    def _():
        lse_out[...] = jnp.zeros_like(lse_out)

    @pl.when(live > 0)
    def _():
        q = q_ref[0]
        lane = lax.broadcasted_iota(jnp.int32, q.shape, 1)
        half = q.shape[1] // 2
        zero = jnp.zeros_like(q)
        queries = jnp.concatenate(
            [jnp.where(lane < half, q, zero), jnp.where(lane >= half, q, zero)], axis=0
        )
        keys = k_ref[0].reshape(-1, k_ref.shape[3])
        values = v_ref[0].reshape(-1, v_ref.shape[3])
        scores = lax.dot_general(
            queries, keys, (((1,), (1,)), ((), ())), preferred_element_type=F32
        )
        column = lax.broadcasted_iota(jnp.int32, scores.shape, 1)
        row = lax.broadcasted_iota(jnp.int32, scores.shape, 0)
        if heads & (heads - 1) == 0:
            same = ((column - row) & (heads - 1)) == 0
        else:
            same = lax.rem(column, heads) == lax.rem(row, heads)
        visible = same & (column < live * heads)
        scores = jnp.where(visible, scores * scale, FLOOR_SCORE)
        peak = jnp.max(scores, axis=1, keepdims=True)
        weights = jnp.exp(scores - peak)
        totals = jnp.sum(weights, axis=1, keepdims=True)
        summed = jnp.dot(weights.astype(BF16), values, preferred_element_type=F32)
        value_out[0] = (summed / totals).astype(BF16)
        lse_out[...] = jnp.where(slot, peak + jnp.log(totals), lse_out[...])

    @pl.when(live <= 0)
    def _():
        value_out[0] = jnp.zeros(value_out.shape[1:], BF16)
        lse_out[...] = jnp.where(slot, FLOOR_SCORE, lse_out[...])


def finish_kernel(
    n, team, heads, owners, tile, width, scale,
    vals, lses, own_qkv, mix, head_gain, tokens, mixer_gain, w_out, w_gate, w_up, w_down,
    out,
    wo, wg, wu, wd, rvals, lsrc, rlses, asrc, agat, xsrc, xdst, ssrc, sdst,
    gsrc, gdst, hsrc, hgat, ysrc, ydst, send, recv, tsend, trecv, load,
):
    me = lax.axis_index("kv")
    mate = lax.axis_index("tp")
    mates = [lax.rem(mate + i, team) for i in range(1, team)]
    barrier, count = greet(n, me, mates)
    hidden_width = w_gate.shape[1]
    loads = [
        pltpu.make_async_copy(w_out, wo, load.at[0]),
        pltpu.make_async_copy(w_gate, wg.at[:, pl.ds(0, hidden_width)], load.at[1]),
        pltpu.make_async_copy(w_up, wu.at[:, pl.ds(0, hidden_width)], load.at[2]),
        pltpu.make_async_copy(w_down, wd, load.at[3]),
    ]
    for copy in loads:
        copy.start()
    padded = owners * tile
    if padded > hidden_width:
        for w in (wg, wu):
            w[:, pl.ds(hidden_width, padded - hidden_width)] = jnp.zeros(
                (w.shape[0], padded - hidden_width), BF16
            )
    seqs = tokens.shape[0]
    first = lax.broadcasted_iota(jnp.int32, (8, LANES), 0) == 0
    for h in range(heads):
        rows = [
            jnp.broadcast_to(lses[pl.ds(m * heads + h, 1), :], (8, LANES)) for m in range(2)
        ]
        lsrc[h] = jnp.where(first, rows[0], rows[1])
    pl.semaphore_wait(barrier, count)

    def vals_copy(o):
        return remote(vals.at[o], rvals.at[me], send.at[0, o], recv.at[0, me], {"kv": o})

    def lses_copy(o):
        return remote(lsrc.at[o], rlses.at[me], send.at[1, o], recv.at[1, me], {"kv": o})

    def attended_copy(o):
        return remote(asrc, agat.at[me], send.at[2, o], recv.at[2, me], {"kv": o})

    def start_parts(o):
        lses_copy(o).start()
        vals_copy(o).start()

    each_owner(n, heads, me, start_parts)

    def own_head():
        rvals[me] = vals[me]
        rlses[me] = lsrc[me]
        q, k, v = (own_qkv[j].astype(F32) for j in range(3))
        product = q * k
        lane = lax.broadcasted_iota(jnp.int32, product.shape, 1)
        half = product.shape[1] // 2
        own_scores = [
            jnp.sum(jnp.where(side, product, 0.0), axis=1, keepdims=True) * scale
            for side in (lane < half, lane >= half)
        ]
        for i in range(1, n):
            landed(rlses, recv.at[1], lax.rem(me + n - i, n))
            landed(rvals, recv.at[0], lax.rem(me + n - i, n))
        normed = []
        for m in range(2):
            own_score = jnp.broadcast_to(own_scores[m], v.shape)
            peak = own_score
            parts = [
                jnp.broadcast_to(to_rows(rlses[j][m : m + 1], seqs), v.shape) for j in range(n)
            ]
            for part in parts:
                peak = jnp.maximum(peak, part)
            own_weight = jnp.exp(own_score - peak)
            totals = own_weight
            summed = own_weight.astype(BF16).astype(F32) * v
            for j in range(n):
                weight = jnp.exp(parts[j] - peak)
                totals = totals + weight
                summed = summed + weight * rvals[j, m].astype(F32)
            normed.append(summed / totals)
        mixture = normed[0] - mix[0, me] * normed[1]
        head_scale = lax.rsqrt(jnp.mean(mixture * mixture, axis=1, keepdims=True) + EPS)
        attended = (mixture * head_scale * head_gain[...]).astype(BF16)
        asrc[...] = attended
        for i in range(1, n):
            attended_copy(lax.rem(me + i, n)).start()
        agat[me] = attended

    when_owner(n, heads, me, own_head)
    loads[0].wait()
    each_owner(n, heads, me, lambda o: landed(agat, recv.at[2], o))
    attended_all = jnp.concatenate([agat[h] for h in range(heads)], axis=1)
    part = jnp.dot(attended_all, wo[...], preferred_element_type=F32).astype(BF16)
    xsrc[...] = part

    def swap_copy(src, dst, phase, other):
        return remote(
            src, dst.at[mate], tsend.at[phase, other], trecv.at[phase, mate], {"tp": other}
        )

    def team_sum(src, dst, phase):
        for other in mates:
            swap_copy(src, dst, phase, other).start()
        total = src[...].astype(F32)
        for other in mates:
            landed(dst, trecv.at[phase], other)
            total = total + dst[other].astype(F32)
        return total

    residual = (tokens[...].astype(F32) + team_sum(xsrc, xdst, 0)).astype(BF16)
    residual_f = residual.astype(F32)
    scaled_mix = (residual_f * mixer_gain[...]).astype(BF16)
    squares = jnp.sum(residual_f * residual_f, axis=1, keepdims=True)
    ssrc[...] = to_lanes(squares)

    def squares_copy(o):
        return remote(ssrc, sdst.at[me], send.at[3, o], recv.at[3, me], {"kv": o})

    def gate_copy(o):
        return remote(gsrc.at[o], gdst.at[me], send.at[4, o], recv.at[4, me], {"kv": o})

    def hidden_copy(o):
        return remote(hsrc, hgat.at[me], send.at[5, o], recv.at[5, me], {"kv": o})

    loads[1].wait()
    loads[2].wait()
    each_owner(n, owners, me, lambda o: squares_copy(o).start())
    for i in range(owners):
        o = lax.rem(me + 1 + i, owners)
        columns = pl.ds(pl.multiple_of(o * tile, LANES), tile)
        for j, w in enumerate((wg, wu)):
            gsrc[o, j] = jnp.dot(
                scaled_mix, w[:, columns], preferred_element_type=F32
            ).astype(BF16)
        pl.when(o != me)(lambda: gate_copy(o).start())

    def own_hidden():
        sdst[me] = ssrc[...]
        gdst[me] = gsrc[me]
        for i in range(1, n):
            landed(sdst, recv.at[3], lax.rem(me + n - i, n))
            landed(gdst, recv.at[4], lax.rem(me + n - i, n))
        total = sdst[0]
        for j in range(1, n):
            total = total + sdst[j]
        inverse = lax.rsqrt(to_rows(total[:1], seqs) / width + EPS)
        gate = gdst[0, 0].astype(F32)
        up = gdst[0, 1].astype(F32)
        for j in range(1, n):
            gate = gate + gdst[j, 0].astype(F32)
            up = up + gdst[j, 1].astype(F32)
        gate = inverse * gate
        hidden = (gate / (1.0 + jnp.exp(-gate)) * (inverse * up)).astype(BF16)
        hsrc[...] = hidden
        for i in range(1, n):
            hidden_copy(lax.rem(me + i, n)).start()
        hgat[me] = hidden

    when_owner(n, owners, me, own_hidden)
    loads[3].wait()
    each_owner(n, owners, me, lambda o: landed(hgat, recv.at[5], o))
    hidden_all = jnp.concatenate([hgat[o] for o in range(owners)], axis=1)[:, :hidden_width]
    down = jnp.dot(hidden_all, wd[...], preferred_element_type=F32).astype(BF16)
    ysrc[...] = down
    out[...] = (residual_f + team_sum(ysrc, ydst, 1)).astype(BF16)

    each_owner(n, heads, me, lambda o: vals_copy(o).wait_send())
    each_owner(n, heads, me, lambda o: lses_copy(o).wait_send())
    for other in mates:
        swap_copy(xsrc, xdst, 0, other).wait_send()
        swap_copy(ysrc, ydst, 1, other).wait_send()
    each_owner(n, owners, me, lambda o: squares_copy(o).wait_send())
    each_owner(n, owners, me, lambda o: gate_copy(o).wait_send())

    def drain(copy):
        for i in range(1, n):
            copy(lax.rem(me + i, n)).wait_send()

    when_owner(n, heads, me, lambda: drain(attended_copy))
    when_owner(n, owners, me, lambda: drain(hidden_copy))


def local(
    n, team, tokens, attn_gain, w_query, w_key, w_value, key_cache, value_cache, lengths,
    mix_weight, head_gain, w_out, mixer_gain, w_gate, w_up, w_down,
):
    seqs, span_width = tokens.shape
    heads = mix_weight.shape[0]
    span = key_cache.shape[1]
    scale = (key_cache.shape[3] // 2) ** -0.5
    width = span_width * n
    hidden_width = w_gate.shape[1]
    tiles = hidden_width // LANES
    tile = -(-tiles // n)
    owners = -(-tiles // tile)
    tile *= LANES
    remote_params = functools.partial(
        pltpu.CompilerParams, has_side_effects=True, vmem_limit_bytes=60 * 2**20
    )

    queries, own_qkv = pl.pallas_call(
        functools.partial(project_kernel, n, heads, width),
        out_shape=(
            jax.ShapeDtypeStruct((heads, seqs, LANES), BF16),
            jax.ShapeDtypeStruct((3, seqs, LANES), BF16),
        ),
        in_specs=[VMEM, VMEM, ANY, ANY, ANY],
        out_specs=(VMEM, VMEM),
        scratch_shapes=[
            pltpu.VMEM((3, *w_query.shape), BF16),
            pltpu.VMEM((heads, 3, seqs, LANES), BF16),
            pltpu.VMEM((n, 3, seqs, LANES), BF16),
            pltpu.VMEM((8, LANES), F32),
            pltpu.VMEM((n, 8, LANES), F32),
            pltpu.VMEM((seqs, LANES), BF16),
            pltpu.VMEM((heads, seqs, LANES), BF16),
            pltpu.SemaphoreType.DMA((3, n)),
            pltpu.SemaphoreType.DMA((3, n)),
            pltpu.SemaphoreType.DMA((3,)),
        ],
        compiler_params=remote_params(collective_id=0),
        name="project",
    )(tokens, attn_gain[None], w_query, w_key, w_value)

    live = lengths - lax.axis_index("kv") * span
    order = jnp.arange(seqs, dtype=jnp.int32)
    seen = (order[None, :] <= order[:, None]) & (live > 0)[None, :]
    fetch = jnp.max(jnp.where(seen, order[None, :], 0), axis=1)
    info = jnp.stack([fetch, live])

    cache_spec = pl.BlockSpec(
        (1, *key_cache.shape[1:]), lambda b, info: (info[0, b], 0, 0, 0)
    )
    part_spec = pl.BlockSpec((1, 2 * heads, LANES), lambda b, info: (b, 0, 0))
    values, lses = pl.pallas_call(
        functools.partial(attend_kernel, heads, scale),
        out_shape=(
            jax.ShapeDtypeStruct((seqs, 2 * heads, LANES), BF16),
            jax.ShapeDtypeStruct((2 * heads, LANES), F32),
        ),
        grid_spec=pltpu.PrefetchScalarGridSpec(
            num_scalar_prefetch=1,
            grid=(seqs,),
            in_specs=[
                pl.BlockSpec((1, heads, LANES), lambda b, info: (b, 0, 0)),
                cache_spec,
                cache_spec,
            ],
            out_specs=(part_spec, pl.BlockSpec((2 * heads, LANES), lambda b, info: (0, 0))),
        ),
        compiler_params=pltpu.CompilerParams(
            dimension_semantics=("arbitrary",), vmem_limit_bytes=60 * 2**20
        ),
        name="attend",
    )(info, queries.transpose(1, 0, 2), key_cache, value_cache)

    def by_head(array):
        return array.reshape(seqs, 2, heads, LANES).transpose(2, 1, 0, 3)

    return pl.pallas_call(
        functools.partial(finish_kernel, n, team, heads, owners, tile, width, scale),
        out_shape=jax.ShapeDtypeStruct((seqs, span_width), BF16),
        in_specs=[VMEM, VMEM, VMEM, SMEM, VMEM, VMEM, VMEM, ANY, ANY, ANY, ANY],
        out_specs=VMEM,
        scratch_shapes=[
            pltpu.VMEM(w_out.shape, BF16),
            pltpu.VMEM((span_width, owners * tile), BF16),
            pltpu.VMEM((span_width, owners * tile), BF16),
            pltpu.VMEM(w_down.shape, BF16),
            pltpu.VMEM((n, 2, seqs, LANES), BF16),
            pltpu.VMEM((heads, 8, LANES), F32),
            pltpu.VMEM((n, 8, LANES), F32),
            pltpu.VMEM((seqs, LANES), BF16),
            pltpu.VMEM((heads, seqs, LANES), BF16),
            pltpu.VMEM((seqs, span_width), BF16),
            pltpu.VMEM((team, seqs, span_width), BF16),
            pltpu.VMEM((8, LANES), F32),
            pltpu.VMEM((n, 8, LANES), F32),
            pltpu.VMEM((owners, 2, seqs, tile), BF16),
            pltpu.VMEM((n, 2, seqs, tile), BF16),
            pltpu.VMEM((seqs, tile), BF16),
            pltpu.VMEM((owners, seqs, tile), BF16),
            pltpu.VMEM((seqs, span_width), BF16),
            pltpu.VMEM((team, seqs, span_width), BF16),
            pltpu.SemaphoreType.DMA((6, n)),
            pltpu.SemaphoreType.DMA((6, n)),
            pltpu.SemaphoreType.DMA((2, team)),
            pltpu.SemaphoreType.DMA((2, team)),
            pltpu.SemaphoreType.DMA((4,)),
        ],
        compiler_params=remote_params(collective_id=1),
        name="finish",
    )(
        by_head(values), lses, own_qkv, mix_weight[None], head_gain[None],
        tokens, mixer_gain[None], w_out, w_gate, w_up, w_down,
    )


def solution(mesh):
    return jax.shard_map(
        functools.partial(local, mesh.shape["kv"], mesh.shape["tp"]),
        mesh=mesh,
        in_specs=(
            P(None, "kv"),
            P("kv"),
            P("kv", "tp"),
            P("kv", "tp"),
            P("kv", "tp"),
            P(None, "kv", "tp", None),
            P(None, "kv", "tp", None),
            P(),
            P("tp"),
            P(),
            P("tp", "kv"),
            P("kv"),
            P("kv", "tp"),
            P("kv", "tp"),
            P("tp", "kv"),
        ),
        out_specs=P(None, "kv"),
        check_vma=False,
    )
```
